768 devices in a mesh: sp: 96 (over z, y), tp: 8 (over x, core).
Axes of the slice: x: 4, y: 8, z: 12, core: 2. Of those that a mesh axis runs over, the one named last changes fastest.
Arguments:
- prompt_input: bfloat16 [27648, 2048], P('sp'), may hold values from -6 to 6
- next_input: bfloat16 [2048], replicated, may hold values from -6 to 6
- norm_gain: float32 [2048], replicated, may hold values from 0.1 to 1.9
- w_key: bfloat16 [2048, 1024], P(None, 'tp'), may hold values from -0.125 to 0.125
- w_value: bfloat16 [2048, 1024], P(None, 'tp'), may hold values from -0.125 to 0.125
- w_query: bfloat16 [2048, 1024], P(None, 'tp'), may hold values from -0.125 to 0.125
- key_offset: float32 [27648, 8], P('sp', 'tp'), may hold values from -10 to 0, as said below
Outputs:
- key_cache: bfloat16 [96, 96, 3, 1024], P('sp', None, None, 'tp')
- value_cache: bfloat16 [96, 96, 3, 1024], P('sp', None, None, 'tp')
- reading: bfloat16 [1024], replicated
The draws below stay inside these ranges and needn't reach their ends.
Inputs may be any that keep to these rules, and one draw needn't show every extreme that they name: `key_offset`: finite log-odds offsets, one per key and head.
All inputs are finite; a program needn't handle non-finite values.
Results may differ from the reference program's by a relative error of at most 0.011.
Values may be sent and summed in bfloat16 or wider, within the bound.
No kernel may reach another device: no remote copies, remote signals or barrier semaphores. Data moves between devices by JAX's collectives and lax.ppermute only.
A program may use at most 32 MiB of HBM per device.

```python
import math
import jax
import jax.numpy as jnp
from jax import lax

D = 2048
HEAD_COUNT = 8
HEAD_DIM = 128
SPAN = 288
PROMPT_LENGTH = 27648
SUB = 3
N_SP = 96


def draw_key_offset(key, part):
    head_order = jax.random.permutation(jax.random.fold_in(key, 11), HEAD_COUNT)
    fast_heads = head_order < HEAD_COUNT // 2
    slow_base = math.log(0.6 / PROMPT_LENGTH)
    fast_base = math.log(0.6 / 40.0)
    base_rate = jnp.where(fast_heads, fast_base, slow_base).astype(jnp.float32)
    block_shift = jax.random.uniform(jax.random.fold_in(key, 12), (HEAD_COUNT, PROMPT_LENGTH // SPAN), jnp.float32, -0.7, 0.7)
    block_shift = jnp.repeat(block_shift, SPAN, axis=1)
    rough_part = jax.random.uniform(jax.random.fold_in(key, 13), (HEAD_COUNT, PROMPT_LENGTH), jnp.float32, -1.0, 1.0)
    offset_table = base_rate[:, None] + block_shift + rough_part
    spike_position = jax.random.randint(jax.random.fold_in(key, 14), (HEAD_COUNT, 3), 0, PROMPT_LENGTH)
    position_slots = jnp.arange(PROMPT_LENGTH, dtype=jnp.int32)
    spike_matches = jnp.any(position_slots[None, None, :] == spike_position[..., None], axis=1)
    signal_level = jax.random.uniform(jax.random.fold_in(key, 15), (HEAD_COUNT, PROMPT_LENGTH), jnp.float32, -1.4, 0.0)
    gradual_mask = jnp.logical_not(fast_heads)[:, None]
    offset_table = jnp.where(jnp.logical_and(spike_matches, gradual_mask), signal_level, offset_table)
    offset_table = jnp.clip(offset_table, -10.0, 0.0)
    return jnp.transpose(offset_table, (1, 0)).astype(jnp.float32)


def steps_of(rng, shape, cuts, least, largest):
    level = 1.0
    for position, parts in cuts:
        steps = jax.random.uniform(jax.random.fold_in(jax.random.fold_in(rng, 6), position), (parts,), jnp.float32, least / len(cuts), largest / len(cuts))
        level = level * jnp.repeat(jnp.exp(steps), shape[position] // parts).reshape((-1,) + (1,) * (len(shape) - 1 - position))
    return level


def noise(key, extent, deviation, most, shards=(), held_as=jnp.bfloat16):
    drawn = deviation * jax.random.normal(key, extent, jnp.float32)
    if shards:
        drawn = drawn * steps_of(key, extent, shards, -0.22, 0.18)
    return jnp.clip(drawn, -most, most).astype(held_as)


def setup_inputs(seed: int = 0) -> dict:
    streams_of = jax.random.split(jax.random.key(seed), 8)
    return {
        "prompt_input": noise(streams_of[0], (PROMPT_LENGTH, D), 1.0, 6.0, ((0, 96),)),
        "next_input": noise(streams_of[1], (D,), 1.0, 6.0),
        "norm_gain": jnp.clip(1.0 + 0.18 * jax.random.normal(streams_of[2], (D,), jnp.float32), 0.1, 1.9),
        "w_key": noise(streams_of[3], (D, HEAD_COUNT * HEAD_DIM), D ** -0.5, 0.125, ((1, 8),)),
        "w_value": noise(streams_of[4], (D, HEAD_COUNT * HEAD_DIM), D ** -0.5, 0.125, ((1, 8),)),
        "w_query": noise(streams_of[5], (D, HEAD_COUNT * HEAD_DIM), D ** -0.5, 0.125, ((1, 8),)),
        "key_offset": draw_key_offset(jax.random.fold_in(streams_of[7], 71), 0),
    }


def norm_rows(row_block, gain_vec):
    wide_rows = row_block.astype(jnp.float32)
    inv_rms = lax.rsqrt(lax.optimization_barrier(jnp.mean(wide_rows * wide_rows, axis=-1, keepdims=True)) + 1e-06)
    return (wide_rows * inv_rms * gain_vec).astype(jnp.bfloat16)

def lay_out(cache_rows):
    blocks = cache_rows.reshape(N_SP, N_SP, SUB, HEAD_COUNT * HEAD_DIM)
    return jnp.transpose(blocks, (1, 0, 2, 3))

def reference(prompt_input, next_input, norm_gain, w_key, w_value, w_query, key_offset):
    normed = norm_rows(prompt_input, norm_gain)
    keys = jnp.dot(normed, w_key, preferred_element_type=jnp.float32).astype(jnp.bfloat16)
    values = jnp.dot(normed, w_value, preferred_element_type=jnp.float32).astype(jnp.bfloat16)
    query_normed = norm_rows(next_input[None, :], norm_gain)
    new_query = jnp.dot(query_normed, w_query, preferred_element_type=jnp.float32).astype(jnp.bfloat16)
    new_query = new_query.reshape(HEAD_COUNT, HEAD_DIM).astype(jnp.float32)
    key_heads = keys.reshape(PROMPT_LENGTH, HEAD_COUNT, HEAD_DIM).astype(jnp.float32)
    value_heads = values.reshape(PROMPT_LENGTH, HEAD_COUNT, HEAD_DIM).astype(jnp.float32)
    logits = jnp.einsum('hd,shd->sh', new_query, key_heads) * HEAD_DIM ** (-0.5) + key_offset
    log_breaks = jax.nn.log_sigmoid(-logits)
    later = lax.cumsum(log_breaks, axis=0, reverse=True) - log_breaks
    weights = jnp.exp(jax.nn.log_sigmoid(logits) + later)
    reading = jnp.einsum('sh,shd->hd', weights, value_heads)
    reading = reading.reshape(HEAD_COUNT * HEAD_DIM).astype(jnp.bfloat16)
    return (lay_out(keys), lay_out(values), reading)
```

```python
import jax
import jax.numpy as jnp
import numpy as np
from jax import lax
from jax.sharding import PartitionSpec as P

HEAD_DIM = 128
SP = "sp"
TP = "tp"
FIRST_RANK = 76


def norm_rows(row_block, gain_vec):
    wide_rows = row_block.astype(jnp.float32)
    inv_rms = lax.rsqrt(jnp.mean(wide_rows * wide_rows, axis=-1, keepdims=True) + 1e-06)
    return (wide_rows * inv_rms * gain_vec).astype(jnp.bfloat16)


def thirds(value):
    high = lax.reduce_precision(value, 8, 7)
    middle = lax.reduce_precision(value - high, 8, 7)
    low = value - high - middle
    return [part.astype(jnp.bfloat16) for part in (high, middle, low)]


def shards(prompt_input, next_input, norm_gain, w_key, w_value, w_query, key_offset):
    span = prompt_input.shape[0]
    slots = lax.axis_size(SP)
    heads = lax.axis_size(TP)
    sub = span // slots
    order = [(r + FIRST_RANK) % slots for r in range(slots)]

    normed = norm_rows(prompt_input, norm_gain)
    keys = jnp.dot(normed, w_key, preferred_element_type=jnp.float32).astype(jnp.bfloat16)
    values = jnp.dot(normed, w_value, preferred_element_type=jnp.float32).astype(jnp.bfloat16)
    query = jnp.dot(norm_rows(next_input[None, :], norm_gain), w_query, preferred_element_type=jnp.float32)
    query = query.astype(jnp.bfloat16)
    logits = lax.dot_general(
        query, keys, (((1,), (1,)), ((), ())), preferred_element_type=jnp.float32
    ) * HEAD_DIM ** (-0.5) + key_offset.reshape(1, span)
    log_breaks = jax.nn.log_sigmoid(-logits)
    inner = lax.cumsum(log_breaks, axis=1, reverse=True) - log_breaks
    total = jnp.sum(log_breaks)
    weights = jnp.exp(jax.nn.log_sigmoid(logits) + inner)
    share = jnp.dot(weights, values.astype(jnp.float32), precision=lax.Precision.HIGHEST)

    turn = lambda rows: jnp.roll(rows.reshape(slots, sub, HEAD_DIM), -FIRST_RANK, axis=0)
    total_row = jnp.concatenate([jnp.stack(thirds(total)), jnp.zeros(HEAD_DIM - 3, jnp.bfloat16)])
    extra = jnp.stack([share[0].astype(jnp.bfloat16), total_row])
    outgoing = jnp.concatenate(
        [turn(keys), turn(values), jnp.broadcast_to(extra[None], (slots, 2, HEAD_DIM))], axis=1
    )
    arrived = lax.all_to_all(
        outgoing, SP, split_axis=0, concat_axis=0, tiled=True, axis_index_groups=[order]
    )
    back = lambda rows: jnp.roll(rows, FIRST_RANK, axis=0)[None]
    key_cache = back(arrived[:, :sub])
    value_cache = back(arrived[:, sub : 2 * sub])

    totals = jnp.sum(arrived[:, 2 * sub + 1, :3].astype(jnp.float32), axis=1)
    place = np.array(order)
    after = jnp.asarray(place[None, :] > place[:, None])
    carried = jnp.sum(jnp.where(after, totals[None, :], 0.0), axis=1)
    shares = arrived[:, 2 * sub].astype(jnp.float32)
    own = jnp.sum(jnp.exp(carried)[:, None] * shares, axis=0).astype(jnp.bfloat16)
    sent = jnp.broadcast_to(own[None, None], (heads, 1, HEAD_DIM))
    reading = lax.all_to_all(sent, TP, split_axis=0, concat_axis=0, tiled=True)
    return key_cache, value_cache, reading.reshape(heads * HEAD_DIM)


def solution(mesh):
    return jax.shard_map(
        shards,
        mesh=mesh,
        in_specs=(P(SP, None), P(), P(), P(None, TP), P(None, TP), P(None, TP), P(SP, TP)),
        out_specs=(P(SP, None, None, TP), P(SP, None, None, TP), P()),
        check_vma=False,
    )
```

```python
import functools

import jax
import jax.numpy as jnp
from jax import lax
from jax.experimental import pallas as pl
from jax.experimental.pallas import tpu as pltpu
from jax.sharding import PartitionSpec as P

HEAD_DIM = 128
LANES = 128
SP = "sp"
TP = "tp"
FIRST_RANK = 76
CHUNK = 96
TP_FIRST = 5


def bf16_parts(value, row, count):
    parts = jnp.zeros_like(value)
    rest = value
    for k in range(count):
        term = rest.astype(jnp.bfloat16).astype(jnp.float32)
        parts = jnp.where(row == k, term, parts)
        rest = rest - term
    return parts.astype(jnp.bfloat16)


def front_kernel(
    x_hbm, next_hbm, gain_hbm, wk_hbm, wv_hbm, wq_hbm, offset_hbm, out_ref,
    x_buf, w_buf, wq_buf, next_buf, gain_buf, offset_buf, normed_buf, k_buf, v_buf, tri_buf, wide_out, sems,
    *, slots, sub,
):
    span, width = x_buf.shape
    chunks = span // CHUNK
    padded = tri_buf.shape[1]
    columns = [pl.ds(c * LANES, LANES) for c in range(width // LANES)]
    copies = {
        "gain": (gain_hbm, gain_buf),
        "x0": (x_hbm.at[pl.ds(0, CHUNK), :], x_buf.at[pl.ds(0, CHUNK), :]),
        "wk": (wk_hbm, w_buf.at[:, pl.ds(0, HEAD_DIM)]),
        "wv": (wv_hbm, w_buf.at[:, pl.ds(HEAD_DIM, HEAD_DIM)]),
        "next": (next_hbm, next_buf),
        "wq": (wq_hbm, wq_buf),
        "offset": (offset_hbm, offset_buf),
    }
    for c in range(1, chunks):
        rows = pl.ds(c * CHUNK, CHUNK)
        copies[f"x{c}"] = (x_hbm.at[rows, :], x_buf.at[rows, :])
    copies = {
        name: pltpu.make_async_copy(source, target, sems.at[number])
        for number, (name, (source, target)) in enumerate(copies.items())
    }
    for copy in copies.values():
        copy.start()

    later = lax.broadcasted_iota(jnp.int32, (span, padded), 0) > lax.broadcasted_iota(jnp.int32, (span, padded), 1)
    beyond = lax.broadcasted_iota(jnp.int32, (span, padded), 1) >= span
    tri_buf[...] = jnp.where(jnp.logical_or(later, beyond), 1.0, 0.0).astype(jnp.bfloat16)

    copies["gain"].wait()
    for c in range(chunks):
        rows = pl.ds(c * CHUNK, CHUNK)
        copies[f"x{c}"].wait()
        squares = jnp.zeros((CHUNK, LANES), jnp.float32)
        for lanes in columns:
            block = x_buf[rows, lanes].astype(jnp.float32)
            squares += block * block
        inv_rms = lax.rsqrt(jnp.sum(squares, axis=1, keepdims=True) * (1.0 / width) + 1e-06)
        for k, lanes in enumerate(columns):
            block = x_buf[rows, lanes].astype(jnp.float32)
            normed_buf[rows, lanes] = (block * inv_rms * gain_buf[k : k + 1, :]).astype(jnp.bfloat16)
        if c == 0:
            copies["wk"].wait()
            copies["wv"].wait()
        both = jnp.dot(normed_buf[rows, :], w_buf[...], preferred_element_type=jnp.float32)
        k_buf[rows, :] = both[:, :HEAD_DIM]
        v_buf[rows, :] = both[:, HEAD_DIM:]

    copies["next"].wait()
    new = next_buf[...].astype(jnp.float32)
    new_inv = lax.rsqrt(jnp.sum(new * new, keepdims=True) * (1.0 / width) + 1e-06)
    new_normed = new * new_inv * gain_buf[...]
    new_row = jnp.concatenate(
        [jnp.broadcast_to(new_normed[k : k + 1, :], (8, LANES)) for k in range(width // LANES)], axis=1
    ).astype(jnp.bfloat16)
    copies["wq"].wait()
    query = jnp.dot(new_row, wq_buf[...], preferred_element_type=jnp.float32).astype(jnp.bfloat16)

    for buf, base in ((k_buf, 0), (v_buf, sub)):
        for k in range(sub):
            for slot, rank, count in (
                (FIRST_RANK, 0, slots - FIRST_RANK),
                (0, slots - FIRST_RANK, FIRST_RANK),
            ):
                wide_out[pl.ds(rank * 8 + base + k, count, stride=8), :] = buf[
                    pl.ds(slot * sub + k, count, stride=sub), :
                ]

    copies["offset"].wait()
    keys = k_buf[...].astype(jnp.bfloat16)
    values = v_buf[...].astype(jnp.bfloat16)
    logits = (
        lax.dot_general(query, keys, (((1,), (1,)), ((), ())), preferred_element_type=jnp.float32)
        * HEAD_DIM ** (-0.5)
        + offset_buf[...]
    )
    row = lax.broadcasted_iota(jnp.int32, (8, span), 0)
    soft = jnp.log1p(jnp.exp(-jnp.abs(logits)))
    log_breaks = -(jnp.maximum(logits, 0.0) + soft)
    log_stops = jnp.minimum(logits, 0.0) - soft
    sums = jnp.sum(
        jnp.dot(bf16_parts(log_breaks, row, 3), tri_buf[...], preferred_element_type=jnp.float32),
        axis=0, keepdims=True,
    )
    weights = jnp.exp(log_stops + sums[:, :span])
    share = jnp.sum(
        jnp.dot(bf16_parts(weights, row, 2), values, preferred_element_type=jnp.float32),
        axis=0, keepdims=True,
    )
    total = sums[:, padded - LANES :]
    lane = lax.broadcasted_iota(jnp.int32, (1, LANES), 1) - (LANES - 3)
    terms = jnp.zeros_like(total)
    rest = total
    for k in range(3):
        term = rest.astype(jnp.bfloat16).astype(jnp.float32)
        terms = jnp.where(lane == k, term, terms)
        rest = rest - term
    wide_out[pl.ds(2 * sub, slots, stride=8), :] = jnp.broadcast_to(share, (slots, LANES))
    wide_out[pl.ds(2 * sub + 1, slots, stride=8), :] = jnp.broadcast_to(terms, (slots, LANES))
    out_ref[...] = wide_out[...].reshape(slots, 8, LANES).astype(jnp.bfloat16)


def front(x, new, gain, w_key, w_value, w_query, offset, slots, sub):
    span, width = x.shape
    padded = -(-(span + 3) // LANES) * LANES
    n_copies = 6 + span // CHUNK
    return pl.pallas_call(
        functools.partial(front_kernel, slots=slots, sub=sub),
        out_shape=pltpu.VMEM((slots, 8, LANES), jnp.bfloat16),
        in_specs=[pl.BlockSpec(memory_space=pl.ANY)] * 7,
        out_specs=pl.BlockSpec(memory_space=pltpu.VMEM),
        scratch_shapes=[
            pltpu.VMEM((span, width), jnp.bfloat16),
            pltpu.VMEM((width, 2 * HEAD_DIM), jnp.bfloat16),
            pltpu.VMEM((width, HEAD_DIM), jnp.bfloat16),
            pltpu.VMEM((width // LANES, LANES), jnp.bfloat16),
            pltpu.VMEM((width // LANES, LANES), jnp.float32),
            pltpu.VMEM((1, span), jnp.float32),
            pltpu.VMEM((span, width), jnp.bfloat16),
            pltpu.VMEM((span, HEAD_DIM), jnp.float32),
            pltpu.VMEM((span, HEAD_DIM), jnp.float32),
            pltpu.VMEM((span, padded), jnp.bfloat16),
            pltpu.VMEM((slots * 8, LANES), jnp.float32),
            pltpu.SemaphoreType.DMA((n_copies,)),
        ],
        name="front",
    )(
        x, new.reshape(width // LANES, LANES), gain.reshape(width // LANES, LANES),
        w_key, w_value, w_query, offset.reshape(1, span),
    )


def join_kernel(arrived_ref, out_ref, wide, *, sub):
    slots = arrived_ref.shape[0]
    wide[...] = arrived_ref[...].astype(jnp.float32).reshape(slots * 8, LANES)
    shares = wide[pl.ds(2 * sub, slots, stride=8), :]
    terms = wide[pl.ds(2 * sub + 1, slots, stride=8), :].astype(jnp.bfloat16)

    def place(dim):
        rank = lax.broadcasted_iota(jnp.int32, (slots, slots), dim)
        return jnp.where(rank < slots - FIRST_RANK, rank + FIRST_RANK, rank + FIRST_RANK - slots)

    after = jnp.where(place(1) > place(0), 1.0, 0.0).astype(jnp.bfloat16)
    carried = jnp.sum(jnp.dot(after, terms, preferred_element_type=jnp.float32), axis=1, keepdims=True)
    own = jnp.sum(jnp.exp(carried) * shares, axis=0, keepdims=True)
    out_ref[...] = jnp.broadcast_to(own[None], out_ref.shape).astype(jnp.bfloat16)


def join(arrived, heads, sub):
    slots = arrived.shape[0]
    return pl.pallas_call(
        functools.partial(join_kernel, sub=sub),
        out_shape=pltpu.VMEM((heads, 1, LANES), jnp.bfloat16),
        in_specs=[pl.BlockSpec(memory_space=pltpu.VMEM)],
        out_specs=pl.BlockSpec(memory_space=pltpu.VMEM),
        scratch_shapes=[pltpu.VMEM((slots * 8, LANES), jnp.float32)],
        name="join",
    )(arrived)


def unpack_kernel(arrived_ref, key_ref, value_ref, wide, cache, *, sub):
    slots = arrived_ref.shape[0]
    wide[...] = arrived_ref[...].astype(jnp.float32).reshape(slots * 8, LANES)
    for out_ref, base in ((key_ref, 0), (value_ref, sub)):
        for k in range(sub):
            for block, rank, count in (
                (FIRST_RANK, 0, slots - FIRST_RANK),
                (0, slots - FIRST_RANK, FIRST_RANK),
            ):
                cache[pl.ds(block, count), :] = wide[pl.ds(rank * 8 + base + k, count, stride=8), :]
            out_ref[k] = cache[...].astype(jnp.bfloat16)


def unpack(arrived, sub):
    slots = arrived.shape[0]
    caches = pl.pallas_call(
        functools.partial(unpack_kernel, sub=sub),
        out_shape=[jax.ShapeDtypeStruct((sub, slots, LANES), jnp.bfloat16)] * 2,
        in_specs=[pl.BlockSpec(memory_space=pltpu.VMEM)],
        out_specs=[pl.BlockSpec(memory_space=pltpu.VMEM)] * 2,
        scratch_shapes=[
            pltpu.VMEM((slots * 8, LANES), jnp.float32),
            pltpu.VMEM((slots, LANES), jnp.float32),
        ],
        name="unpack",
    )(arrived)
    return [cache.transpose(1, 0, 2)[None] for cache in caches]


def finish_kernel(heads_ref, out_ref):
    heads = out_ref.shape[0]
    for r in range(heads):
        h = (r + TP_FIRST) % heads
        out_ref[h : h + 1, :] = heads_ref[r]


def finish(heads_read):
    heads = heads_read.shape[0]
    return pl.pallas_call(
        finish_kernel,
        out_shape=jax.ShapeDtypeStruct((heads, LANES), jnp.bfloat16),
        in_specs=[pl.BlockSpec(memory_space=pltpu.VMEM)],
        out_specs=pl.BlockSpec(memory_space=pltpu.VMEM),
        name="finish",
    )(heads_read).reshape(heads * LANES)


def on_chip(array):
    return pltpu.with_memory_space_constraint(array, pltpu.VMEM)


def shards(prompt_input, next_input, norm_gain, w_key, w_value, w_query, key_offset):
    span = prompt_input.shape[0]
    slots = lax.axis_size(SP)
    heads = lax.axis_size(TP)
    sub = span // slots
    order = [(r + FIRST_RANK) % slots for r in range(slots)]

    outgoing = front(prompt_input, next_input, norm_gain, w_key, w_value, w_query, key_offset, slots, sub)
    arrived = lax.all_to_all(
        outgoing, SP, split_axis=0, concat_axis=0, tiled=True, axis_index_groups=[order]
    )
    arrived = on_chip(arrived)
    own = join( arrived, heads, sub)
    tp_order = [(r + TP_FIRST) % heads for r in range(heads)]
    reading = lax.all_to_all(own, TP, split_axis=0, concat_axis=0, tiled=True, axis_index_groups=[tp_order])
    return *unpack(arrived, sub), finish(on_chip(reading))


def solution(mesh):
    return jax.shard_map(
        shards,
        mesh=mesh,
        in_specs=(P(SP, None), P(), P(), P(None, TP), P(None, TP), P(None, TP), P(SP, TP)),
        out_specs=(P(SP, None, None, TP), P(SP, None, None, TP), P()),
        check_vma=False,
    )
```

```python
import functools

import jax
import jax.numpy as jnp
from jax import lax
from jax.experimental import pallas as pl
from jax.experimental.pallas import tpu as pltpu
from jax.sharding import PartitionSpec as P

HEAD_DIM = 128
LANES = 128
SP = "sp"
TP = "tp"
FIRST_RANK = 76
CHUNK = 96
SLICE = 2048
TP_FIRST = 5


def bf16_parts(value, row, count):
    parts = jnp.zeros_like(value)
    rest = value
    for k in range(count):
        term = rest.astype(jnp.bfloat16).astype(jnp.float32)
        parts = jnp.where(row == k, term, parts)
        rest = rest - term
    return parts.astype(jnp.bfloat16)


def front_kernel(
    x_hbm, next_hbm, gain_hbm, wk_hbm, wv_hbm, wq_hbm, offset_hbm, out_ref,
    x_buf, w_buf, wq_buf, next_buf, gain_buf, offset_buf, normed_buf, k_buf, v_buf, tri_buf, wide_out, sems,
    *, slots, sub,
):
    span, width = x_buf.shape
    padded = tri_buf.shape[1]
    row_blocks = [pl.ds(c * CHUNK, CHUNK) for c in range(span // CHUNK)]
    slices = [pl.ds(c * SLICE, SLICE) for c in range(width // SLICE)]
    columns = [pl.ds(c * LANES, LANES) for c in range(width // LANES)]

    sources = [(gain_hbm, gain_buf), (next_hbm, next_buf), (offset_hbm, offset_buf), (wq_hbm, wq_buf)]
    sources += [(x_hbm.at[rows, :], x_buf.at[rows, :]) for rows in row_blocks]
    for rows in slices:
        sources += [(wk_hbm.at[rows, :], w_buf.at[rows, pl.ds(0, HEAD_DIM)])]
        sources += [(wv_hbm.at[rows, :], w_buf.at[rows, pl.ds(HEAD_DIM, HEAD_DIM)])]
    copies = [pltpu.make_async_copy(source, target, sems.at[n]) for n, (source, target) in enumerate(sources)]
    for copy in copies:
        copy.start()
    gain_copy, next_copy, offset_copy, wq_copy, *more = copies
    x_copies, w_copies = more[: len(row_blocks)], more[len(row_blocks) :]

    later = lax.broadcasted_iota(jnp.int32, (span, padded), 0) > lax.broadcasted_iota(jnp.int32, (span, padded), 1)
    beyond = lax.broadcasted_iota(jnp.int32, (span, padded), 1) >= span
    tri_buf[...] = jnp.where(jnp.logical_or(later, beyond), 1.0, 0.0).astype(jnp.bfloat16)

    gain_copy.wait()
    next_copy.wait()
    new = next_buf[...].astype(jnp.float32)
    new_inv = lax.rsqrt(jnp.sum(new * new, keepdims=True) * (1.0 / width) + 1e-06)
    new_normed = new * new_inv * gain_buf[...]
    new_row = jnp.concatenate(
        [jnp.broadcast_to(new_normed[k : k + 1, :], (8, LANES)) for k in range(width // LANES)], axis=1
    ).astype(jnp.bfloat16)
    offset_copy.wait()
    wq_copy.wait()
    query = jnp.dot(new_row, wq_buf[...], preferred_element_type=jnp.float32).astype(jnp.bfloat16)

    for rows, copy in zip(row_blocks, x_copies):
        copy.wait()
        squares = jnp.zeros((CHUNK, LANES), jnp.float32)
        for lanes in columns:
            block = x_buf[rows, lanes].astype(jnp.float32)
            squares += block * block
        inv_rms = lax.rsqrt(jnp.sum(squares, axis=1, keepdims=True) * (1.0 / width) + 1e-06)
        for k, lanes in enumerate(columns):
            block = x_buf[rows, lanes].astype(jnp.float32)
            normed_buf[rows, lanes] = (block * inv_rms * gain_buf[k : k + 1, :]).astype(jnp.bfloat16)

    w_copies[0].wait()
    w_copies[1].wait()
    both = jnp.concatenate([
        jnp.dot(normed_buf[r : r + 144, :], w_buf[...], preferred_element_type=jnp.float32)
        for r in range(0, span, 144)
    ], axis=0)
    k_buf[...] = both[:, :HEAD_DIM]
    v_buf[...] = both[:, HEAD_DIM:]
    keys = both[:, :HEAD_DIM].astype(jnp.bfloat16)
    values = both[:, HEAD_DIM:].astype(jnp.bfloat16)
    logits = (
        lax.dot_general(query, keys, (((1,), (1,)), ((), ())), preferred_element_type=jnp.float32)
        * HEAD_DIM ** (-0.5)
        + offset_buf[...]
    )
    row = lax.broadcasted_iota(jnp.int32, (8, span), 0)
    soft = jnp.log1p(jnp.exp(-jnp.abs(logits)))
    log_breaks = -(jnp.maximum(logits, 0.0) + soft)
    log_stops = jnp.minimum(logits, 0.0) - soft
    sums = jnp.sum(
        jnp.dot(bf16_parts(log_breaks, row, 3), tri_buf[...], preferred_element_type=jnp.float32),
        axis=0, keepdims=True,
    )
    weights = jnp.exp(log_stops + sums[:, :span])
    share = jnp.sum(
        jnp.dot(bf16_parts(weights, row, 2), values, preferred_element_type=jnp.float32),
        axis=0, keepdims=True,
    )

    for buf, base in ((k_buf, 0), (v_buf, sub)):
        for k in range(sub):
            for slot, rank, count in (
                (FIRST_RANK, 0, slots - FIRST_RANK),
                (0, slots - FIRST_RANK, FIRST_RANK),
            ):
                wide_out[pl.ds(rank * 8 + base + k, count, stride=8), :] = buf[
                    pl.ds(slot * sub + k, count, stride=sub), :
                ]

    total = sums[:, padded - LANES :]
    lane = lax.broadcasted_iota(jnp.int32, (1, LANES), 1) - (LANES - 3)
    terms = jnp.zeros_like(total)
    rest = total
    for k in range(3):
        term = rest.astype(jnp.bfloat16).astype(jnp.float32)
        terms = jnp.where(lane == k, term, terms)
        rest = rest - term
    wide_out[pl.ds(2 * sub, slots, stride=8), :] = jnp.broadcast_to(share, (slots, LANES))
    wide_out[pl.ds(2 * sub + 1, slots, stride=8), :] = jnp.broadcast_to(terms, (slots, LANES))
    out_ref[...] = wide_out[...].reshape(slots, 8, LANES).astype(jnp.bfloat16)


def front(x, new, gain, w_key, w_value, w_query, offset, slots, sub):
    span, width = x.shape
    padded = -(-(span + 3) // LANES) * LANES
    n_copies = 4 + span // CHUNK + 2 * (width // SLICE)
    return pl.pallas_call(
        functools.partial(front_kernel, slots=slots, sub=sub),
        out_shape=pltpu.VMEM((slots, 8, LANES), jnp.bfloat16),
        in_specs=[pl.BlockSpec(memory_space=pl.ANY)] * 7,
        out_specs=pl.BlockSpec(memory_space=pltpu.VMEM),
        scratch_shapes=[
            pltpu.VMEM((span, width), jnp.bfloat16),
            pltpu.VMEM((width, 2 * HEAD_DIM), jnp.bfloat16),
            pltpu.VMEM((width, HEAD_DIM), jnp.bfloat16),
            pltpu.VMEM((width // LANES, LANES), jnp.bfloat16),
            pltpu.VMEM((width // LANES, LANES), jnp.float32),
            pltpu.VMEM((1, span), jnp.float32),
            pltpu.VMEM((span, width), jnp.bfloat16),
            pltpu.VMEM((span, HEAD_DIM), jnp.float32),
            pltpu.VMEM((span, HEAD_DIM), jnp.float32),
            pltpu.VMEM((span, padded), jnp.bfloat16),
            pltpu.VMEM((slots * 8, LANES), jnp.float32),
            pltpu.SemaphoreType.DMA((n_copies,)),
        ],
        name="front",
    )(
        x, new.reshape(width // LANES, LANES), gain.reshape(width // LANES, LANES),
        w_key, w_value, w_query, offset.reshape(1, span),
    )


def join_kernel(arrived_ref, out_ref, wide, *, sub):
    slots = arrived_ref.shape[0]
    wide[...] = arrived_ref[...].astype(jnp.float32).reshape(slots * 8, LANES)
    shares = wide[pl.ds(2 * sub, slots, stride=8), :]
    terms = wide[pl.ds(2 * sub + 1, slots, stride=8), :].astype(jnp.bfloat16)

    def place(dim):
        rank = lax.broadcasted_iota(jnp.int32, (slots, slots), dim)
        return jnp.where(rank < slots - FIRST_RANK, rank + FIRST_RANK, rank + FIRST_RANK - slots)

    after = jnp.where(place(1) > place(0), 1.0, 0.0).astype(jnp.bfloat16)
    carried = jnp.sum(jnp.dot(after, terms, preferred_element_type=jnp.float32), axis=1, keepdims=True)
    own = jnp.sum(jnp.exp(carried) * shares, axis=0, keepdims=True)
    out_ref[...] = jnp.broadcast_to(own[None], out_ref.shape).astype(jnp.bfloat16)


def join(arrived, heads, sub):
    slots = arrived.shape[0]
    return pl.pallas_call(
        functools.partial(join_kernel, sub=sub),
        out_shape=pltpu.VMEM((heads, 1, LANES), jnp.bfloat16),
        in_specs=[pl.BlockSpec(memory_space=pltpu.VMEM)],
        out_specs=pl.BlockSpec(memory_space=pltpu.VMEM),
        scratch_shapes=[pltpu.VMEM((slots * 8, LANES), jnp.float32)],
        name="join",
    )(arrived)


def unpack_kernel(arrived_ref, key_ref, value_ref, wide, cache, *, sub):
    slots = arrived_ref.shape[0]
    wide[...] = arrived_ref[...].astype(jnp.float32).reshape(slots * 8, LANES)
    for out_ref, base in ((key_ref, 0), (value_ref, sub)):
        for k in range(sub):
            for block, rank, count in (
                (FIRST_RANK, 0, slots - FIRST_RANK),
                (0, slots - FIRST_RANK, FIRST_RANK),
            ):
                cache[pl.ds(block, count), :] = wide[pl.ds(rank * 8 + base + k, count, stride=8), :]
            out_ref[k] = cache[...].astype(jnp.bfloat16)


def unpack(arrived, sub):
    slots = arrived.shape[0]
    caches = pl.pallas_call(
        functools.partial(unpack_kernel, sub=sub),
        out_shape=[jax.ShapeDtypeStruct((sub, slots, LANES), jnp.bfloat16)] * 2,
        in_specs=[pl.BlockSpec(memory_space=pltpu.VMEM)],
        out_specs=[pl.BlockSpec(memory_space=pltpu.VMEM)] * 2,
        scratch_shapes=[
            pltpu.VMEM((slots * 8, LANES), jnp.float32),
            pltpu.VMEM((slots, LANES), jnp.float32),
        ],
        name="unpack",
    )(arrived)
    return [cache.transpose(1, 0, 2)[None] for cache in caches]


def finish_kernel(heads_ref, out_ref):
    heads = out_ref.shape[0]
    for r in range(heads):
        h = (r + TP_FIRST) % heads
        out_ref[h : h + 1, :] = heads_ref[r]


def finish(heads_read):
    heads = heads_read.shape[0]
    return pl.pallas_call(
        finish_kernel,
        out_shape=jax.ShapeDtypeStruct((heads, LANES), jnp.bfloat16),
        in_specs=[pl.BlockSpec(memory_space=pltpu.VMEM)],
        out_specs=pl.BlockSpec(memory_space=pltpu.VMEM),
        name="finish",
    )(heads_read).reshape(heads * LANES)


def on_chip(array):
    return pltpu.with_memory_space_constraint(array, pltpu.VMEM)


def shards(prompt_input, next_input, norm_gain, w_key, w_value, w_query, key_offset):
    span = prompt_input.shape[0]
    slots = lax.axis_size(SP)
    heads = lax.axis_size(TP)
    sub = span // slots
    order = [(r + FIRST_RANK) % slots for r in range(slots)]

    outgoing = front(prompt_input, next_input, norm_gain, w_key, w_value, w_query, key_offset, slots, sub)
    arrived = lax.all_to_all(
        outgoing, SP, split_axis=0, concat_axis=0, tiled=True, axis_index_groups=[order]
    )
    arrived = on_chip(arrived)
    own = join( arrived, heads, sub)
    tp_order = [(r + TP_FIRST) % heads for r in range(heads)]
    reading = lax.all_to_all(own, TP, split_axis=0, concat_axis=0, tiled=True, axis_index_groups=[tp_order])
    return *unpack(arrived, sub), finish(on_chip(reading))


def solution(mesh):
    return jax.shard_map(
        shards,
        mesh=mesh,
        in_specs=(P(SP, None), P(), P(), P(None, TP), P(None, TP), P(None, TP), P(SP, TP)),
        out_specs=(P(SP, None, None, TP), P(SP, None, None, TP), P()),
        check_vma=False,
    )
```

```python
import functools

import jax
import jax.numpy as jnp
from jax import lax
from jax.experimental import pallas as pl
from jax.experimental.pallas import tpu as pltpu
from jax.sharding import PartitionSpec as P

HEAD_DIM = 128
LANES = 128
SP = "sp"
TP = "tp"
FIRST_RANK = 68
CHUNK = 96
TP_FIRST = 5


def bf16_parts(value, row, count):
    parts = jnp.zeros_like(value)
    rest = value
    for k in range(count):
        term = rest.astype(jnp.bfloat16).astype(jnp.float32)
        parts = jnp.where(row == k, term, parts)
        rest = rest - term
    return parts.astype(jnp.bfloat16)


def front_kernel(
    x_hbm, next_hbm, gain_hbm, wk_hbm, wv_hbm, wq_hbm, offset_hbm, out_ref,
    x_buf, w_buf, wq_buf, next_buf, gain_buf, offset_buf, normed_buf, k_buf, v_buf, tri_buf, wide_out, sems,
    *, slots, sub,
):
    span, width = x_buf.shape
    padded = tri_buf.shape[1]
    row_blocks = [pl.ds(c * CHUNK, CHUNK) for c in range(span // CHUNK)]
    columns = [pl.ds(c * LANES, LANES) for c in range(width // LANES)]

    sources = [(gain_hbm, gain_buf), (next_hbm, next_buf), (offset_hbm, offset_buf), (wq_hbm, wq_buf)]
    sources += [(x_hbm.at[rows, :], x_buf.at[rows, :]) for rows in row_blocks]
    sources += [(wk_hbm, w_buf.at[:, pl.ds(0, HEAD_DIM)]), (wv_hbm, w_buf.at[:, pl.ds(HEAD_DIM, HEAD_DIM)])]
    copies = [pltpu.make_async_copy(source, target, sems.at[n]) for n, (source, target) in enumerate(sources)]
    for copy in copies:
        copy.start()
    gain_copy, next_copy, offset_copy, wq_copy, *more = copies
    x_copies, w_copies = more[: len(row_blocks)], more[len(row_blocks) :]

    later = lax.broadcasted_iota(jnp.int32, (span, padded), 0) > lax.broadcasted_iota(jnp.int32, (span, padded), 1)
    beyond = lax.broadcasted_iota(jnp.int32, (span, padded), 1) >= span
    tri_buf[...] = jnp.where(jnp.logical_or(later, beyond), 1.0, 0.0).astype(jnp.bfloat16)

    gain_copy.wait()
    next_copy.wait()
    new = next_buf[...].astype(jnp.float32)
    new_inv = lax.rsqrt(jnp.sum(new * new, keepdims=True) * (1.0 / width) + 1e-06)
    new_normed = new * new_inv * gain_buf[...]
    new_row = jnp.concatenate(
        [jnp.broadcast_to(new_normed[k : k + 1, :], (8, LANES)) for k in range(width // LANES)], axis=1
    ).astype(jnp.bfloat16)
    offset_copy.wait()
    wq_copy.wait()
    query = jnp.dot(new_row, wq_buf[...], preferred_element_type=jnp.float32).astype(jnp.bfloat16)

    for rows, copy in zip(row_blocks, x_copies):
        copy.wait()
        squares = jnp.zeros((CHUNK, LANES), jnp.float32)
        for lanes in columns:
            block = x_buf[rows, lanes].astype(jnp.float32)
            squares += block * block
        inv_rms = lax.rsqrt(jnp.sum(squares, axis=1, keepdims=True) * (1.0 / width) + 1e-06)
        for k, lanes in enumerate(columns):
            block = x_buf[rows, lanes].astype(jnp.float32)
            normed_buf[rows, lanes] = (block * inv_rms * gain_buf[k : k + 1, :]).astype(jnp.bfloat16)

    w_copies[0].wait()
    w_copies[1].wait()
    both = jnp.concatenate([
        jnp.dot(normed_buf[r : r + 144, :], w_buf[...], preferred_element_type=jnp.float32)
        for r in range(0, span, 144)
    ], axis=0)
    k_buf[:span, :] = both[:, :HEAD_DIM]
    v_buf[:span, :] = both[:, HEAD_DIM:]
    keys = both[:, :HEAD_DIM].astype(jnp.bfloat16)
    values = both[:, HEAD_DIM:].astype(jnp.bfloat16)
    logits = (
        lax.dot_general(query, keys, (((1,), (1,)), ((), ())), preferred_element_type=jnp.float32)
        * HEAD_DIM ** (-0.5)
        + offset_buf[...]
    )
    row = lax.broadcasted_iota(jnp.int32, (8, span), 0)
    soft = jnp.log1p(jnp.exp(-jnp.abs(logits)))
    log_breaks = -(jnp.maximum(logits, 0.0) + soft)
    log_stops = jnp.minimum(logits, 0.0) - soft
    sums = jnp.sum(
        jnp.dot(bf16_parts(log_breaks, row, 3), tri_buf[...], preferred_element_type=jnp.float32),
        axis=0, keepdims=True,
    )
    weights = jnp.exp(log_stops + sums[:, :span])
    share = jnp.sum(
        jnp.dot(bf16_parts(weights, row, 2), values, preferred_element_type=jnp.float32),
        axis=0, keepdims=True,
    )

    for buf, base in ((k_buf, 0), (v_buf, sub)):
        for k in range(sub):
            for slot, rank, count in (
                (FIRST_RANK, 0, slots - FIRST_RANK),
                (0, slots - FIRST_RANK, FIRST_RANK),
            ):
                wide_out[pl.ds(rank * 8 + base + k, count, stride=8), :] = buf[
                    pl.ds(slot * sub + k, count, stride=sub), :
                ]

    total = sums[:, padded - LANES :]
    lane = lax.broadcasted_iota(jnp.int32, (1, LANES), 1) - (LANES - 3)
    terms = jnp.zeros_like(total)
    rest = total
    for k in range(3):
        term = rest.astype(jnp.bfloat16).astype(jnp.float32)
        terms = jnp.where(lane == k, term, terms)
        rest = rest - term
    wide_out[pl.ds(2 * sub, slots, stride=8), :] = jnp.broadcast_to(share, (slots, LANES))
    wide_out[pl.ds(2 * sub + 1, slots, stride=8), :] = jnp.broadcast_to(terms, (slots, LANES))
    out_ref[...] = wide_out[: slots * 8, :].reshape(slots, 8, LANES).astype(jnp.bfloat16)


def front(x, new, gain, w_key, w_value, w_query, offset, slots, sub):
    span, width = x.shape
    padded = -(-(span + 3) // LANES) * LANES
    n_copies = 6 + span // CHUNK
    return pl.pallas_call(
        functools.partial(front_kernel, slots=slots, sub=sub),
        out_shape=pltpu.VMEM((slots, 8, LANES), jnp.bfloat16),
        in_specs=[pl.BlockSpec(memory_space=pl.ANY)] * 7,
        out_specs=pl.BlockSpec(memory_space=pltpu.VMEM),
        scratch_shapes=[
            pltpu.VMEM((span, width), jnp.bfloat16),
            pltpu.VMEM((width, 2 * HEAD_DIM), jnp.bfloat16),
            pltpu.VMEM((width, HEAD_DIM), jnp.bfloat16),
            pltpu.VMEM((width // LANES, LANES), jnp.bfloat16),
            pltpu.VMEM((width // LANES, LANES), jnp.float32),
            pltpu.VMEM((1, span), jnp.float32),
            pltpu.VMEM((span, width), jnp.bfloat16),
            pltpu.VMEM((span + 8 * sub, HEAD_DIM), jnp.float32),
            pltpu.VMEM((span + 8 * sub, HEAD_DIM), jnp.float32),
            pltpu.VMEM((span, padded), jnp.bfloat16),
            pltpu.VMEM((slots * 8 + 64, LANES), jnp.float32),
            pltpu.SemaphoreType.DMA((n_copies,)),
        ],
        name="front",
    )(
        x, new.reshape(width // LANES, LANES), gain.reshape(width // LANES, LANES),
        w_key, w_value, w_query, offset.reshape(1, span),
    )


def join_kernel(arrived_ref, out_ref, wide, *, sub):
    slots = arrived_ref.shape[0]
    wide[...] = arrived_ref[...].astype(jnp.float32).reshape(slots * 8, LANES)
    shares = wide[pl.ds(2 * sub, slots, stride=8), :]
    terms = wide[pl.ds(2 * sub + 1, slots, stride=8), :].astype(jnp.bfloat16)

    def place(dim):
        rank = lax.broadcasted_iota(jnp.int32, (slots, slots), dim)
        return jnp.where(rank < slots - FIRST_RANK, rank + FIRST_RANK, rank + FIRST_RANK - slots)

    after = jnp.where(place(1) > place(0), 1.0, 0.0).astype(jnp.bfloat16)
    carried = jnp.sum(jnp.dot(after, terms, preferred_element_type=jnp.float32), axis=1, keepdims=True)
    own = jnp.sum(jnp.exp(carried) * shares, axis=0, keepdims=True)
    out_ref[...] = jnp.broadcast_to(own[None], out_ref.shape).astype(jnp.bfloat16)


def join(arrived, heads, sub):
    slots = arrived.shape[0]
    return pl.pallas_call(
        functools.partial(join_kernel, sub=sub),
        out_shape=pltpu.VMEM((heads, 1, LANES), jnp.bfloat16),
        in_specs=[pl.BlockSpec(memory_space=pltpu.VMEM)],
        out_specs=pl.BlockSpec(memory_space=pltpu.VMEM),
        scratch_shapes=[pltpu.VMEM((slots * 8, LANES), jnp.float32)],
        name="join",
    )(arrived)


def finish_kernel(heads_ref, arrived_ref, read_ref, key_ref, value_ref, wide, cache, *, sub):
    slots = arrived_ref.shape[0]
    heads = read_ref.shape[0]
    for r in range(heads):
        h = (r + TP_FIRST) % heads
        read_ref[h : h + 1, :] = heads_ref[r]
    wide[: slots * 8, :] = arrived_ref[...].astype(jnp.float32).reshape(slots * 8, LANES)
    for out_ref, base in ((key_ref, 0), (value_ref, sub)):
        for k in range(sub):
            for block, rank, count in (
                (FIRST_RANK, 0, slots - FIRST_RANK),
                (0, slots - FIRST_RANK, FIRST_RANK),
            ):
                cache[pl.ds(block, count), :] = wide[pl.ds(rank * 8 + base + k, count, stride=8), :]
            out_ref[k] = cache[:slots, :].astype(jnp.bfloat16)


def finish(heads_read, arrived, sub):
    heads = heads_read.shape[0]
    slots = arrived.shape[0]
    read, *caches = pl.pallas_call(
        functools.partial(finish_kernel, sub=sub),
        out_shape=[jax.ShapeDtypeStruct((heads, LANES), jnp.bfloat16)]
        + [jax.ShapeDtypeStruct((sub, slots, LANES), jnp.bfloat16)] * 2,
        in_specs=[pl.BlockSpec(memory_space=pltpu.VMEM)] * 2,
        out_specs=[pl.BlockSpec(memory_space=pltpu.VMEM)] * 3,
        scratch_shapes=[
            pltpu.VMEM((slots * 8 + 64, LANES), jnp.float32),
            pltpu.VMEM((slots + 8, LANES), jnp.float32),
        ],
        name="finish",
    )(heads_read, arrived)
    return *[cache.transpose(1, 0, 2)[None] for cache in caches], read.reshape(heads * LANES)


def on_chip(array):
    return pltpu.with_memory_space_constraint(array, pltpu.VMEM)


def shards(prompt_input, next_input, norm_gain, w_key, w_value, w_query, key_offset):
    span = prompt_input.shape[0]
    slots = lax.axis_size(SP)
    heads = lax.axis_size(TP)
    sub = span // slots
    order = [(r + FIRST_RANK) % slots for r in range(slots)]

    outgoing = front(prompt_input, next_input, norm_gain, w_key, w_value, w_query, key_offset, slots, sub)
    arrived = lax.all_to_all(
        outgoing, SP, split_axis=0, concat_axis=0, tiled=True, axis_index_groups=[order]
    )
    arrived = on_chip(arrived)
    own = join( arrived, heads, sub)
    tp_order = [(r + TP_FIRST) % heads for r in range(heads)]
    reading = lax.all_to_all(own, TP, split_axis=0, concat_axis=0, tiled=True, axis_index_groups=[tp_order])
    return finish(on_chip(reading), arrived, sub)


def solution(mesh):
    return jax.shard_map(
        shards,
        mesh=mesh,
        in_specs=(P(SP, None), P(), P(), P(None, TP), P(None, TP), P(None, TP), P(SP, TP)),
        out_specs=(P(SP, None, None, TP), P(SP, None, None, TP), P()),
        check_vma=False,
    )
```

```python
import functools

import jax
import jax.numpy as jnp
from jax import lax
from jax.experimental import pallas as pl
from jax.experimental.pallas import tpu as pltpu
from jax.sharding import PartitionSpec as P

HEAD_DIM = 128
LANES = 128
SP = "sp"
TP = "tp"
FIRST_RANK = 68
CHUNK = 96
TP_FIRST = 5


def bf16_parts(value, row, count):
    parts = jnp.zeros_like(value)
    rest = value
    for k in range(count):
        term = rest.astype(jnp.bfloat16).astype(jnp.float32)
        parts = jnp.where(row == k, term, parts)
        rest = rest - term
    return parts.astype(jnp.bfloat16)


def front_kernel(
    x_hbm, next_hbm, gain_hbm, wk_hbm, wv_hbm, wq_hbm, offset_hbm, out_ref,
    x_buf, w_buf, wq_buf, next_buf, gain_buf, offset_buf, normed_buf, k_buf, v_buf, tri_buf, wide_out, sems,
    *, slots, sub,
):
    span, width = x_buf.shape
    padded = tri_buf.shape[1]
    row_blocks = [pl.ds(c * CHUNK, CHUNK) for c in range(span // CHUNK)]
    columns = [pl.ds(c * LANES, LANES) for c in range(width // LANES)]

    sources = [(gain_hbm, gain_buf), (next_hbm, next_buf), (offset_hbm, offset_buf)]
    sources += [(x_hbm.at[rows, :], x_buf.at[rows, :]) for rows in row_blocks]
    sources += [(wk_hbm, w_buf.at[:, pl.ds(0, HEAD_DIM)]), (wv_hbm, w_buf.at[:, pl.ds(HEAD_DIM, HEAD_DIM)])]
    sources += [(wq_hbm, wq_buf)]
    copies = [pltpu.make_async_copy(source, target, sems.at[n]) for n, (source, target) in enumerate(sources)]
    for copy in copies:
        copy.start()
    gain_copy, next_copy, offset_copy, *more, wq_copy = copies
    x_copies, w_copies = more[: len(row_blocks)], more[len(row_blocks) :]

    later = lax.broadcasted_iota(jnp.int32, (span, padded), 0) > lax.broadcasted_iota(jnp.int32, (span, padded), 1)
    beyond = lax.broadcasted_iota(jnp.int32, (span, padded), 1) >= span
    tri_buf[...] = jnp.where(jnp.logical_or(later, beyond), 1.0, 0.0).astype(jnp.bfloat16)

    gain_copy.wait()
    next_copy.wait()
    new = next_buf[...].astype(jnp.float32)
    new_inv = lax.rsqrt(jnp.sum(new * new, keepdims=True) * (1.0 / width) + 1e-06)
    new_normed = new * new_inv * gain_buf[...]
    new_row = jnp.concatenate(
        [jnp.broadcast_to(new_normed[k : k + 1, :], (8, LANES)) for k in range(width // LANES)], axis=1
    ).astype(jnp.bfloat16)
    offset_copy.wait()

    for rows, copy in zip(row_blocks, x_copies):
        copy.wait()
        squares = jnp.zeros((CHUNK, LANES), jnp.float32)
        for lanes in columns:
            block = x_buf[rows, lanes].astype(jnp.float32)
            squares += block * block
        inv_rms = lax.rsqrt(jnp.sum(squares, axis=1, keepdims=True) * (1.0 / width) + 1e-06)
        for k, lanes in enumerate(columns):
            block = x_buf[rows, lanes].astype(jnp.float32)
            normed_buf[rows, lanes] = (block * inv_rms * gain_buf[k : k + 1, :]).astype(jnp.bfloat16)

    w_copies[0].wait()
    w_copies[1].wait()
    halves = [pl.ds(r, span // 2) for r in (0, span // 2)]
    upper = jnp.dot(normed_buf[halves[0], :], w_buf[...], preferred_element_type=jnp.float32)
    lower = jnp.dot(normed_buf[halves[1], :], w_buf[...], preferred_element_type=jnp.float32)
    wq_copy.wait()
    query = jnp.dot(new_row, wq_buf[...], preferred_element_type=jnp.float32).astype(jnp.bfloat16)
    both = jnp.concatenate([upper, lower], axis=0)
    k_buf[:span, :] = both[:, :HEAD_DIM]
    v_buf[:span, :] = both[:, HEAD_DIM:]
    keys = both[:, :HEAD_DIM].astype(jnp.bfloat16)
    values = both[:, HEAD_DIM:].astype(jnp.bfloat16)
    logits = (
        lax.dot_general(query, keys, (((1,), (1,)), ((), ())), preferred_element_type=jnp.float32)
        * HEAD_DIM ** (-0.5)
        + offset_buf[...]
    )
    row = lax.broadcasted_iota(jnp.int32, (8, span), 0)
    soft = jnp.log1p(jnp.exp(-jnp.abs(logits)))
    log_breaks = -(jnp.maximum(logits, 0.0) + soft)
    log_stops = jnp.minimum(logits, 0.0) - soft
    sums = jnp.sum(
        jnp.dot(bf16_parts(log_breaks, row, 3), tri_buf[...], preferred_element_type=jnp.float32),
        axis=0, keepdims=True,
    )
    weights = jnp.exp(log_stops + sums[:, :span])
    share = jnp.sum(
        jnp.dot(bf16_parts(weights, row, 2), values, preferred_element_type=jnp.float32),
        axis=0, keepdims=True,
    )

    for buf, base in ((k_buf, 0), (v_buf, sub)):
        for k in range(sub):
            for slot, rank, count in (
                (FIRST_RANK, 0, slots - FIRST_RANK),
                (0, slots - FIRST_RANK, FIRST_RANK),
            ):
                wide_out[pl.ds(rank * 8 + base + k, count, stride=8), :] = buf[
                    pl.ds(slot * sub + k, count, stride=sub), :
                ]

    total = sums[:, padded - LANES :]
    lane = lax.broadcasted_iota(jnp.int32, (1, LANES), 1) - (LANES - 3)
    terms = jnp.zeros_like(total)
    rest = total
    for k in range(3):
        term = rest.astype(jnp.bfloat16).astype(jnp.float32)
        terms = jnp.where(lane == k, term, terms)
        rest = rest - term
    wide_out[pl.ds(2 * sub, slots, stride=8), :] = jnp.broadcast_to(share, (slots, LANES))
    wide_out[pl.ds(2 * sub + 1, slots, stride=8), :] = jnp.broadcast_to(terms, (slots, LANES))
    out_ref[...] = wide_out[: slots * 8, :].reshape(slots, 8, LANES).astype(jnp.bfloat16)


def front(x, new, gain, w_key, w_value, w_query, offset, slots, sub):
    span, width = x.shape
    padded = -(-(span + 3) // LANES) * LANES
    n_copies = 6 + span // CHUNK
    return pl.pallas_call(
        functools.partial(front_kernel, slots=slots, sub=sub),
        out_shape=pltpu.VMEM((slots, 8, LANES), jnp.bfloat16),
        in_specs=[pl.BlockSpec(memory_space=pl.ANY)] * 7,
        out_specs=pl.BlockSpec(memory_space=pltpu.VMEM),
        scratch_shapes=[
            pltpu.VMEM((span, width), jnp.bfloat16),
            pltpu.VMEM((width, 2 * HEAD_DIM), jnp.bfloat16),
            pltpu.VMEM((width, HEAD_DIM), jnp.bfloat16),
            pltpu.VMEM((width // LANES, LANES), jnp.bfloat16),
            pltpu.VMEM((width // LANES, LANES), jnp.float32),
            pltpu.VMEM((1, span), jnp.float32),
            pltpu.VMEM((span, width), jnp.bfloat16),
            pltpu.VMEM((span + 8 * sub, HEAD_DIM), jnp.float32),
            pltpu.VMEM((span + 8 * sub, HEAD_DIM), jnp.float32),
            pltpu.VMEM((span, padded), jnp.bfloat16),
            pltpu.VMEM((slots * 8 + 64, LANES), jnp.float32),
            pltpu.SemaphoreType.DMA((n_copies,)),
        ],
        name="front",
    )(
        x, new.reshape(width // LANES, LANES), gain.reshape(width // LANES, LANES),
        w_key, w_value, w_query, offset.reshape(1, span),
    )


def join_kernel(arrived_ref, out_ref, wide, *, sub):
    slots = arrived_ref.shape[0]
    wide[...] = arrived_ref[...].astype(jnp.float32).reshape(slots * 8, LANES)
    shares = wide[pl.ds(2 * sub, slots, stride=8), :]
    terms = wide[pl.ds(2 * sub + 1, slots, stride=8), :].astype(jnp.bfloat16)

    def place(dim):
        rank = lax.broadcasted_iota(jnp.int32, (slots, slots), dim)
        return jnp.where(rank < slots - FIRST_RANK, rank + FIRST_RANK, rank + FIRST_RANK - slots)

    after = jnp.where(place(1) > place(0), 1.0, 0.0).astype(jnp.bfloat16)
    carried = jnp.sum(jnp.dot(after, terms, preferred_element_type=jnp.float32), axis=1, keepdims=True)
    own = jnp.sum(jnp.exp(carried) * shares, axis=0, keepdims=True)
    out_ref[...] = jnp.broadcast_to(own[None], out_ref.shape).astype(jnp.bfloat16)


def join(arrived, heads, sub):
    slots = arrived.shape[0]
    return pl.pallas_call(
        functools.partial(join_kernel, sub=sub),
        out_shape=pltpu.VMEM((heads, 1, LANES), jnp.bfloat16),
        in_specs=[pl.BlockSpec(memory_space=pltpu.VMEM)],
        out_specs=pl.BlockSpec(memory_space=pltpu.VMEM),
        scratch_shapes=[pltpu.VMEM((slots * 8, LANES), jnp.float32)],
        name="join",
    )(arrived)


def finish_kernel(heads_ref, arrived_ref, read_ref, key_ref, value_ref, wide, cache, *, sub):
    slots = arrived_ref.shape[0]
    heads = read_ref.shape[0]
    for r in range(heads):
        h = (r + TP_FIRST) % heads
        read_ref[h : h + 1, :] = heads_ref[r]
    wide[: slots * 8, :] = arrived_ref[...].astype(jnp.float32).reshape(slots * 8, LANES)
    for out_ref, base in ((key_ref, 0), (value_ref, sub)):
        for k in range(sub):
            for block, rank, count in (
                (FIRST_RANK, 0, slots - FIRST_RANK),
                (0, slots - FIRST_RANK, FIRST_RANK),
            ):
                cache[pl.ds(block, count), :] = wide[pl.ds(rank * 8 + base + k, count, stride=8), :]
            out_ref[k] = cache[:slots, :].astype(jnp.bfloat16)


def finish(heads_read, arrived, sub):
    heads = heads_read.shape[0]
    slots = arrived.shape[0]
    read, *caches = pl.pallas_call(
        functools.partial(finish_kernel, sub=sub),
        out_shape=[jax.ShapeDtypeStruct((heads, LANES), jnp.bfloat16)]
        + [jax.ShapeDtypeStruct((sub, slots, LANES), jnp.bfloat16)] * 2,
        in_specs=[pl.BlockSpec(memory_space=pltpu.VMEM)] * 2,
        out_specs=[pl.BlockSpec(memory_space=pltpu.VMEM)] * 3,
        scratch_shapes=[
            pltpu.VMEM((slots * 8 + 64, LANES), jnp.float32),
            pltpu.VMEM((slots + 8, LANES), jnp.float32),
        ],
        name="finish",
    )(heads_read, arrived)
    return *[cache.transpose(1, 0, 2)[None] for cache in caches], read.reshape(heads * LANES)


def on_chip(array):
    return pltpu.with_memory_space_constraint(array, pltpu.VMEM)


def shards(prompt_input, next_input, norm_gain, w_key, w_value, w_query, key_offset):
    span = prompt_input.shape[0]
    slots = lax.axis_size(SP)
    heads = lax.axis_size(TP)
    sub = span // slots
    order = [(r + FIRST_RANK) % slots for r in range(slots)]

    outgoing = front(prompt_input, next_input, norm_gain, w_key, w_value, w_query, key_offset, slots, sub)
    arrived = lax.all_to_all(
        outgoing, SP, split_axis=0, concat_axis=0, tiled=True, axis_index_groups=[order]
    )
    arrived = on_chip(arrived)
    own = join( arrived, heads, sub)
    tp_order = [(r + TP_FIRST) % heads for r in range(heads)]
    reading = lax.all_to_all(own, TP, split_axis=0, concat_axis=0, tiled=True, axis_index_groups=[tp_order])
    return finish(on_chip(reading), arrived, sub)


def solution(mesh):
    return jax.shard_map(
        shards,
        mesh=mesh,
        in_specs=(P(SP, None), P(), P(), P(None, TP), P(None, TP), P(None, TP), P(SP, TP)),
        out_specs=(P(SP, None, None, TP), P(SP, None, None, TP), P()),
        check_vma=False,
    )
```

```python
import functools

import jax
import jax.numpy as jnp
from jax import lax
from jax.experimental import pallas as pl
from jax.experimental.pallas import tpu as pltpu
from jax.sharding import PartitionSpec as P

HEAD_DIM = 128
LANES = 128
SP = "sp"
TP = "tp"
FIRST_RANK = 68
CHUNK = 96
TP_FIRST = 5


def bf16_parts(value, row, count):
    parts = jnp.zeros_like(value)
    rest = value
    for k in range(count):
        term = rest.astype(jnp.bfloat16).astype(jnp.float32)
        parts = jnp.where(row == k, term, parts)
        rest = rest - term
    return parts.astype(jnp.bfloat16)


def front_kernel(
    x_hbm, next_hbm, gain_hbm, wk_hbm, wv_hbm, wq_hbm, offset_hbm, out_ref,
    x_buf, w_buf, wq_buf, next_buf, gain_buf, offset_buf, normed_buf, k_buf, v_buf, tri_buf, wide_out, sems,
    *, slots, sub,
):
    span, width = x_buf.shape
    padded = tri_buf.shape[1]
    row_blocks = [pl.ds(c * CHUNK, CHUNK) for c in range(span // CHUNK)]
    columns = [pl.ds(c * LANES, LANES) for c in range(width // LANES)]

    sources = [(gain_hbm, gain_buf), (next_hbm, next_buf), (offset_hbm, offset_buf)]
    sources += [(x_hbm.at[rows, :], x_buf.at[rows, :]) for rows in row_blocks]
    sources += [(wk_hbm, w_buf.at[:, pl.ds(0, HEAD_DIM)]), (wv_hbm, w_buf.at[:, pl.ds(HEAD_DIM, HEAD_DIM)])]
    sources += [(wq_hbm, wq_buf)]
    copies = [pltpu.make_async_copy(source, target, sems.at[n]) for n, (source, target) in enumerate(sources)]
    for copy in copies:
        copy.start()
    gain_copy, next_copy, offset_copy, *more, wq_copy = copies
    x_copies, w_copies = more[: len(row_blocks)], more[len(row_blocks) :]

    later = lax.broadcasted_iota(jnp.int32, (span, padded), 0) > lax.broadcasted_iota(jnp.int32, (span, padded), 1)
    beyond = lax.broadcasted_iota(jnp.int32, (span, padded), 1) >= span
    tri_buf[...] = jnp.where(jnp.logical_or(later, beyond), 1.0, 0.0).astype(jnp.bfloat16)

    gain_copy.wait()
    next_copy.wait()
    new = next_buf[...].astype(jnp.float32)
    new_inv = lax.rsqrt(jnp.sum(new * new, keepdims=True) * (1.0 / width) + 1e-06)
    new_normed = new * new_inv * gain_buf[...]
    new_row = jnp.concatenate(
        [jnp.broadcast_to(new_normed[k : k + 1, :], (8, LANES)) for k in range(width // LANES)], axis=1
    ).astype(jnp.bfloat16)
    offset_copy.wait()

    for rows, copy in zip(row_blocks, x_copies):
        copy.wait()
        squares = jnp.zeros((CHUNK, LANES), jnp.float32)
        for lanes in columns:
            block = x_buf[rows, lanes].astype(jnp.float32)
            squares += block * block
        inv_rms = lax.rsqrt(jnp.sum(squares, axis=1, keepdims=True) * (1.0 / width) + 1e-06)
        for k, lanes in enumerate(columns):
            block = x_buf[rows, lanes].astype(jnp.float32)
            normed_buf[rows, lanes] = (block * inv_rms * gain_buf[k : k + 1, :]).astype(jnp.bfloat16)

    w_copies[0].wait()
    w_copies[1].wait()
    halves = [pl.ds(r, span // 2) for r in (0, span // 2)]
    upper = jnp.dot(normed_buf[halves[0], :], w_buf[...], preferred_element_type=jnp.float32)
    lower = jnp.dot(normed_buf[halves[1], :], w_buf[...], preferred_element_type=jnp.float32)
    wq_copy.wait()
    query = jnp.dot(new_row, wq_buf[...], preferred_element_type=jnp.float32).astype(jnp.bfloat16)
    both = jnp.concatenate([upper, lower], axis=0)
    k_buf[:span, :] = both[:, :HEAD_DIM]
    v_buf[:span, :] = both[:, HEAD_DIM:]
    keys = both[:, :HEAD_DIM].astype(jnp.bfloat16)
    values = both[:, HEAD_DIM:].astype(jnp.bfloat16)
    logits = (
        lax.dot_general(query, keys, (((1,), (1,)), ((), ())), preferred_element_type=jnp.float32)
        * HEAD_DIM ** (-0.5)
        + offset_buf[...]
    )
    row = lax.broadcasted_iota(jnp.int32, (8, span), 0)
    soft = jnp.log1p(jnp.exp(-jnp.abs(logits)))
    log_breaks = -(jnp.maximum(logits, 0.0) + soft)
    log_stops = jnp.minimum(logits, 0.0) - soft
    sums = jnp.sum(
        jnp.dot(bf16_parts(log_breaks, row, 3), tri_buf[...], preferred_element_type=jnp.float32),
        axis=0, keepdims=True,
    )
    weights = jnp.exp(log_stops + sums[:, :span])
    share = jnp.sum(
        jnp.dot(bf16_parts(weights, row, 2), values, preferred_element_type=jnp.float32),
        axis=0, keepdims=True,
    )

    for buf, base in ((k_buf, 0), (v_buf, sub)):
        for k in range(sub):
            for slot, rank, count in (
                (FIRST_RANK, 0, slots - FIRST_RANK),
                (0, slots - FIRST_RANK, FIRST_RANK),
            ):
                wide_out[pl.ds(rank * 8 + base + k, count, stride=8), :] = buf[
                    pl.ds(slot * sub + k, count, stride=sub), :
                ]

    total = sums[:, padded - LANES :]
    lane = lax.broadcasted_iota(jnp.int32, (1, LANES), 1) - (LANES - 3)
    terms = jnp.zeros_like(total)
    rest = total
    for k in range(3):
        term = rest.astype(jnp.bfloat16).astype(jnp.float32)
        terms = jnp.where(lane == k, term, terms)
        rest = rest - term
    wide_out[pl.ds(2 * sub, slots, stride=8), :] = jnp.broadcast_to(share, (slots, LANES))
    wide_out[pl.ds(2 * sub + 1, slots, stride=8), :] = jnp.broadcast_to(terms, (slots, LANES))
    out_ref[...] = wide_out[: slots * 8, :].reshape(slots, 8, LANES).astype(jnp.bfloat16)


def front(x, new, gain, w_key, w_value, w_query, offset, slots, sub):
    span, width = x.shape
    padded = -(-(span + 3) // LANES) * LANES
    n_copies = 6 + span // CHUNK
    return pl.pallas_call(
        functools.partial(front_kernel, slots=slots, sub=sub),
        out_shape=pltpu.VMEM((slots, 8, LANES), jnp.bfloat16),
        in_specs=[pl.BlockSpec(memory_space=pl.ANY)] * 7,
        out_specs=pl.BlockSpec(memory_space=pltpu.VMEM),
        scratch_shapes=[
            pltpu.VMEM((span, width), jnp.bfloat16),
            pltpu.VMEM((width, 2 * HEAD_DIM), jnp.bfloat16),
            pltpu.VMEM((width, HEAD_DIM), jnp.bfloat16),
            pltpu.VMEM((width // LANES, LANES), jnp.bfloat16),
            pltpu.VMEM((width // LANES, LANES), jnp.float32),
            pltpu.VMEM((1, span), jnp.float32),
            pltpu.VMEM((span, width), jnp.bfloat16),
            pltpu.VMEM((span + 8 * sub, HEAD_DIM), jnp.float32),
            pltpu.VMEM((span + 8 * sub, HEAD_DIM), jnp.float32),
            pltpu.VMEM((span, padded), jnp.bfloat16),
            pltpu.VMEM((slots * 8 + 64, LANES), jnp.float32),
            pltpu.SemaphoreType.DMA((n_copies,)),
        ],
        name="front",
    )(
        x, new.reshape(width // LANES, LANES), gain.reshape(width // LANES, LANES),
        w_key, w_value, w_query, offset.reshape(1, span),
    )


def unpack(wide, packed, sub):
    slots = packed.shape[1]
    for c in range(2 * sub):
        low = wide[pl.ds((slots - FIRST_RANK) * 8 + c, FIRST_RANK, stride=8), :]
        high = wide[pl.ds(c, slots - FIRST_RANK, stride=8), :]
        packed[c] = jnp.concatenate([low, high], axis=0).astype(jnp.bfloat16)


def join_kernel(arrived_ref, out_ref, packed_ref, wide, *, sub):
    slots = arrived_ref.shape[0]
    wide[: slots * 8, :] = arrived_ref[...].astype(jnp.float32).reshape(slots * 8, LANES)
    shares = wide[pl.ds(2 * sub, slots, stride=8), :]
    terms = wide[pl.ds(2 * sub + 1, slots, stride=8), :].astype(jnp.bfloat16)

    def place(dim):
        rank = lax.broadcasted_iota(jnp.int32, (slots, slots), dim)
        return jnp.where(rank < slots - FIRST_RANK, rank + FIRST_RANK, rank + FIRST_RANK - slots)

    after = jnp.where(place(1) > place(0), 1.0, 0.0).astype(jnp.bfloat16)
    carried = jnp.sum(jnp.dot(after, terms, preferred_element_type=jnp.float32), axis=1, keepdims=True)
    own = jnp.sum(jnp.exp(carried) * shares, axis=0, keepdims=True)
    out_ref[...] = jnp.broadcast_to(own[None], out_ref.shape).astype(jnp.bfloat16)

    @pl.when(lax.rem(lax.axis_index(TP), 2) == 1)
    def _():
        unpack(wide, packed_ref, sub)


def join(arrived, heads, sub):
    slots = arrived.shape[0]
    return pl.pallas_call(
        functools.partial(join_kernel, sub=sub),
        out_shape=[
            pltpu.VMEM((heads, 1, LANES), jnp.bfloat16),
            pltpu.VMEM((2 * sub, slots, LANES), jnp.bfloat16),
        ],
        in_specs=[pl.BlockSpec(memory_space=pltpu.VMEM)],
        out_specs=[pl.BlockSpec(memory_space=pltpu.VMEM)] * 2,
        scratch_shapes=[pltpu.VMEM((slots * 8 + 64, LANES), jnp.float32)],
        name="join",
    )(arrived)


def finish_kernel(heads_ref, arrived_ref, packed_ref, read_hbm, key_hbm, value_hbm, read_buf, wide, packed_here, sems, *, sub):
    slots = arrived_ref.shape[0]
    heads = read_buf.shape[0]
    odd = lax.rem(lax.axis_index(TP), 2) == 1

    def caches_from(packed):
        return [
            pltpu.make_async_copy(packed.at[pl.ds(c * sub, sub)], target, sems.at[c])
            for c, target in enumerate((key_hbm, value_hbm))
        ]

    @pl.when(odd)
    def _():
        for copy in caches_from(packed_ref):
            copy.start()

    for r in range(heads):
        h = (r + TP_FIRST) % heads
        read_buf[h : h + 1, :] = heads_ref[r]
    read_copy = pltpu.make_async_copy(read_buf, read_hbm, sems.at[2])
    read_copy.start()

    @pl.when(jnp.logical_not(odd))
    def _():
        wide[: slots * 8, :] = arrived_ref[...].astype(jnp.float32).reshape(slots * 8, LANES)
        unpack(wide, packed_here, sub)
        for copy in caches_from(packed_here):
            copy.start()

    for copy in caches_from(packed_here):
        copy.wait()
    read_copy.wait()


def finish(heads_read, arrived, packed, sub):
    heads = heads_read.shape[0]
    slots = arrived.shape[0]
    read, *caches = pl.pallas_call(
        functools.partial(finish_kernel, sub=sub),
        out_shape=[jax.ShapeDtypeStruct((heads, LANES), jnp.bfloat16)]
        + [jax.ShapeDtypeStruct((sub, slots, LANES), jnp.bfloat16)] * 2,
        in_specs=[pl.BlockSpec(memory_space=pltpu.VMEM)] * 3,
        out_specs=[pl.BlockSpec(memory_space=pl.ANY)] * 3,
        scratch_shapes=[
            pltpu.VMEM((heads, LANES), jnp.bfloat16),
            pltpu.VMEM((slots * 8 + 64, LANES), jnp.float32),
            pltpu.VMEM((2 * sub, slots, LANES), jnp.bfloat16),
            pltpu.SemaphoreType.DMA((3,)),
        ],
        name="finish",
    )(heads_read, arrived, packed)
    return *[cache.transpose(1, 0, 2)[None] for cache in caches], read.reshape(heads * LANES)


def on_chip(array):
    return pltpu.with_memory_space_constraint(array, pltpu.VMEM)


def shards(prompt_input, next_input, norm_gain, w_key, w_value, w_query, key_offset):
    span = prompt_input.shape[0]
    slots = lax.axis_size(SP)
    heads = lax.axis_size(TP)
    sub = span // slots
    order = [(r + FIRST_RANK) % slots for r in range(slots)]

    outgoing = front(prompt_input, next_input, norm_gain, w_key, w_value, w_query, key_offset, slots, sub)
    arrived = lax.all_to_all(
        outgoing, SP, split_axis=0, concat_axis=0, tiled=True, axis_index_groups=[order]
    )
    arrived = on_chip(arrived)
    own, packed = join(arrived, heads, sub)
    tp_order = [(r + TP_FIRST) % heads for r in range(heads)]
    reading = lax.all_to_all(own, TP, split_axis=0, concat_axis=0, tiled=True, axis_index_groups=[tp_order])
    return finish(on_chip(reading), arrived, on_chip(packed), sub)


def solution(mesh):
    return jax.shard_map(
        shards,
        mesh=mesh,
        in_specs=(P(SP, None), P(), P(), P(None, TP), P(None, TP), P(None, TP), P(SP, TP)),
        out_specs=(P(SP, None, None, TP), P(SP, None, None, TP), P()),
        check_vma=False,
    )
```

```python
import functools

import jax
import jax.numpy as jnp
from jax import lax
from jax.experimental import pallas as pl
from jax.experimental.pallas import tpu as pltpu
from jax.sharding import PartitionSpec as P

HEAD_DIM = 128
LANES = 128
SP = "sp"
TP = "tp"
FIRST_RANK = 68
CHUNK = 96
TP_FIRST = 5


def bf16_parts(value, row, count):
    parts = jnp.zeros_like(value)
    rest = value
    for k in range(count):
        term = rest.astype(jnp.bfloat16).astype(jnp.float32)
        parts = jnp.where(row == k, term, parts)
        rest = rest - term
    return parts.astype(jnp.bfloat16)


def front_kernel(
    x_hbm, next_hbm, gain_hbm, wk_hbm, wv_hbm, wq_hbm, offset_hbm, out_ref,
    x_buf, w_buf, wq_buf, next_buf, gain_buf, offset_buf, normed_buf, k_buf, v_buf, tri_buf, wide_out, sems,
    *, slots, sub,
):
    span, width = x_buf.shape
    padded = tri_buf.shape[1]
    row_blocks = [pl.ds(c * CHUNK, CHUNK) for c in range(span // CHUNK)]
    columns = [pl.ds(c * LANES, LANES) for c in range(width // LANES)]

    sources = [(gain_hbm, gain_buf), (next_hbm, next_buf), (offset_hbm, offset_buf)]
    sources += [(x_hbm.at[rows, :], x_buf.at[rows, :]) for rows in row_blocks]
    sources += [(wk_hbm, w_buf.at[:, pl.ds(0, HEAD_DIM)]), (wv_hbm, w_buf.at[:, pl.ds(HEAD_DIM, HEAD_DIM)])]
    sources += [(wq_hbm, wq_buf)]
    copies = [pltpu.make_async_copy(source, target, sems.at[n]) for n, (source, target) in enumerate(sources)]
    for copy in copies:
        copy.start()
    gain_copy, next_copy, offset_copy, *more, wq_copy = copies
    x_copies, w_copies = more[: len(row_blocks)], more[len(row_blocks) :]

    later = lax.broadcasted_iota(jnp.int32, (span, padded), 0) > lax.broadcasted_iota(jnp.int32, (span, padded), 1)
    beyond = lax.broadcasted_iota(jnp.int32, (span, padded), 1) >= span
    tri_buf[...] = jnp.where(jnp.logical_or(later, beyond), 1.0, 0.0).astype(jnp.bfloat16)

    gain_copy.wait()
    next_copy.wait()
    new = next_buf[...].astype(jnp.float32)
    new_inv = lax.rsqrt(jnp.sum(new * new, keepdims=True) * (1.0 / width) + 1e-06)
    new_normed = new * new_inv * gain_buf[...]
    new_row = jnp.concatenate(
        [jnp.broadcast_to(new_normed[k : k + 1, :], (8, LANES)) for k in range(width // LANES)], axis=1
    ).astype(jnp.bfloat16)
    offset_copy.wait()

    for rows, copy in zip(row_blocks, x_copies):
        copy.wait()
        squares = jnp.zeros((CHUNK, LANES), jnp.float32)
        for lanes in columns:
            block = x_buf[rows, lanes].astype(jnp.float32)
            squares += block * block
        inv_rms = lax.rsqrt(jnp.sum(squares, axis=1, keepdims=True) * (1.0 / width) + 1e-06)
        for k, lanes in enumerate(columns):
            block = x_buf[rows, lanes].astype(jnp.float32)
            normed_buf[rows, lanes] = (block * inv_rms * gain_buf[k : k + 1, :]).astype(jnp.bfloat16)

    w_copies[0].wait()
    w_copies[1].wait()
    halves = [pl.ds(r, span // 2) for r in (0, span // 2)]
    upper = jnp.dot(normed_buf[halves[0], :], w_buf[...], preferred_element_type=jnp.float32)
    lower = jnp.dot(normed_buf[halves[1], :], w_buf[...], preferred_element_type=jnp.float32)
    wq_copy.wait()
    query = jnp.dot(new_row, wq_buf[...], preferred_element_type=jnp.float32).astype(jnp.bfloat16)
    both = jnp.concatenate([upper, lower], axis=0)
    k_buf[:span, :] = both[:, :HEAD_DIM]
    v_buf[:span, :] = both[:, HEAD_DIM:]
    for buf, base in ((k_buf, 0), (v_buf, sub)):
        for k in range(sub):
            for slot, rank, count in (
                (FIRST_RANK, 0, slots - FIRST_RANK),
                (0, slots - FIRST_RANK, FIRST_RANK),
            ):
                wide_out[pl.ds(rank * 8 + base + k, count, stride=8), :] = buf[
                    pl.ds(slot * sub + k, count, stride=sub), :
                ]

    keys = both[:, :HEAD_DIM].astype(jnp.bfloat16)
    values = both[:, HEAD_DIM:].astype(jnp.bfloat16)
    logits = (
        lax.dot_general(query, keys, (((1,), (1,)), ((), ())), preferred_element_type=jnp.float32)
        * HEAD_DIM ** (-0.5)
        + offset_buf[...]
    )
    row = lax.broadcasted_iota(jnp.int32, (8, span), 0)
    soft = jnp.log1p(jnp.exp(-jnp.abs(logits)))
    log_breaks = -(jnp.maximum(logits, 0.0) + soft)
    log_stops = jnp.minimum(logits, 0.0) - soft
    sums = jnp.sum(
        jnp.dot(bf16_parts(log_breaks, row, 3), tri_buf[...], preferred_element_type=jnp.float32),
        axis=0, keepdims=True,
    )
    weights = jnp.exp(log_stops + sums[:, :span])
    share = jnp.sum(
        jnp.dot(bf16_parts(weights, row, 2), values, preferred_element_type=jnp.float32),
        axis=0, keepdims=True,
    )

    total = sums[:, padded - LANES :]
    lane = lax.broadcasted_iota(jnp.int32, (1, LANES), 1) - (LANES - 3)
    terms = jnp.zeros_like(total)
    rest = total
    for k in range(3):
        term = rest.astype(jnp.bfloat16).astype(jnp.float32)
        terms = jnp.where(lane == k, term, terms)
        rest = rest - term
    wide_out[pl.ds(2 * sub, slots, stride=8), :] = jnp.broadcast_to(share, (slots, LANES))
    wide_out[pl.ds(2 * sub + 1, slots, stride=8), :] = jnp.broadcast_to(terms, (slots, LANES))
    out_ref[...] = wide_out[: slots * 8, :].reshape(slots, 8, LANES).astype(jnp.bfloat16)


def front(x, new, gain, w_key, w_value, w_query, offset, slots, sub):
    span, width = x.shape
    padded = -(-(span + 3) // LANES) * LANES
    n_copies = 6 + span // CHUNK
    return pl.pallas_call(
        functools.partial(front_kernel, slots=slots, sub=sub),
        out_shape=pltpu.VMEM((slots, 8, LANES), jnp.bfloat16),
        in_specs=[pl.BlockSpec(memory_space=pl.ANY)] * 7,
        out_specs=pl.BlockSpec(memory_space=pltpu.VMEM),
        scratch_shapes=[
            pltpu.VMEM((span, width), jnp.bfloat16),
            pltpu.VMEM((width, 2 * HEAD_DIM), jnp.bfloat16),
            pltpu.VMEM((width, HEAD_DIM), jnp.bfloat16),
            pltpu.VMEM((width // LANES, LANES), jnp.bfloat16),
            pltpu.VMEM((width // LANES, LANES), jnp.float32),
            pltpu.VMEM((1, span), jnp.float32),
            pltpu.VMEM((span, width), jnp.bfloat16),
            pltpu.VMEM((span + 8 * sub, HEAD_DIM), jnp.float32),
            pltpu.VMEM((span + 8 * sub, HEAD_DIM), jnp.float32),
            pltpu.VMEM((span, padded), jnp.bfloat16),
            pltpu.VMEM((slots * 8 + 64, LANES), jnp.float32),
            pltpu.SemaphoreType.DMA((n_copies,)),
        ],
        name="front",
    )(
        x, new.reshape(width // LANES, LANES), gain.reshape(width // LANES, LANES),
        w_key, w_value, w_query, offset.reshape(1, span),
    )


def join_kernel(arrived_ref, out_ref, wide, *, sub):
    slots = arrived_ref.shape[0]
    wide[...] = arrived_ref[...].astype(jnp.float32).reshape(slots * 8, LANES)
    shares = wide[pl.ds(2 * sub, slots, stride=8), :]
    terms = wide[pl.ds(2 * sub + 1, slots, stride=8), :].astype(jnp.bfloat16)

    def place(dim):
        rank = lax.broadcasted_iota(jnp.int32, (slots, slots), dim)
        return jnp.where(rank < slots - FIRST_RANK, rank + FIRST_RANK, rank + FIRST_RANK - slots)

    after = jnp.where(place(1) > place(0), 1.0, 0.0).astype(jnp.bfloat16)
    carried = jnp.sum(jnp.dot(after, terms, preferred_element_type=jnp.float32), axis=1, keepdims=True)
    own = jnp.sum(jnp.exp(carried) * shares, axis=0, keepdims=True)
    out_ref[...] = jnp.broadcast_to(own[None], out_ref.shape).astype(jnp.bfloat16)


def join(arrived, heads, sub):
    slots = arrived.shape[0]
    return pl.pallas_call(
        functools.partial(join_kernel, sub=sub),
        out_shape=pltpu.VMEM((heads, 1, LANES), jnp.bfloat16),
        in_specs=[pl.BlockSpec(memory_space=pltpu.VMEM)],
        out_specs=pl.BlockSpec(memory_space=pltpu.VMEM),
        scratch_shapes=[pltpu.VMEM((slots * 8, LANES), jnp.float32)],
        name="join",
    )(arrived)


def finish_kernel(heads_ref, arrived_ref, read_ref, key_ref, value_ref, wide, cache, *, sub):
    slots = arrived_ref.shape[0]
    heads = read_ref.shape[0]
    for r in range(heads):
        h = (r + TP_FIRST) % heads
        read_ref[h : h + 1, :] = heads_ref[r]
    wide[: slots * 8, :] = arrived_ref[...].astype(jnp.float32).reshape(slots * 8, LANES)
    for out_ref, base in ((key_ref, 0), (value_ref, sub)):
        for k in range(sub):
            for block, rank, count in (
                (FIRST_RANK, 0, slots - FIRST_RANK),
                (0, slots - FIRST_RANK, FIRST_RANK),
            ):
                cache[pl.ds(block, count), :] = wide[pl.ds(rank * 8 + base + k, count, stride=8), :]
            out_ref[k] = cache[:slots, :].astype(jnp.bfloat16)


def finish(heads_read, arrived, sub):
    heads = heads_read.shape[0]
    slots = arrived.shape[0]
    read, *caches = pl.pallas_call(
        functools.partial(finish_kernel, sub=sub),
        out_shape=[jax.ShapeDtypeStruct((heads, LANES), jnp.bfloat16)]
        + [jax.ShapeDtypeStruct((sub, slots, LANES), jnp.bfloat16)] * 2,
        in_specs=[pl.BlockSpec(memory_space=pltpu.VMEM)] * 2,
        out_specs=[pl.BlockSpec(memory_space=pltpu.VMEM)] * 3,
        scratch_shapes=[
            pltpu.VMEM((slots * 8 + 64, LANES), jnp.float32),
            pltpu.VMEM((slots + 8, LANES), jnp.float32),
        ],
        name="finish",
    )(heads_read, arrived)
    return *[cache.transpose(1, 0, 2)[None] for cache in caches], read.reshape(heads * LANES)


def on_chip(array):
    return pltpu.with_memory_space_constraint(array, pltpu.VMEM)


def shards(prompt_input, next_input, norm_gain, w_key, w_value, w_query, key_offset):
    span = prompt_input.shape[0]
    slots = lax.axis_size(SP)
    heads = lax.axis_size(TP)
    sub = span // slots
    order = [(r + FIRST_RANK) % slots for r in range(slots)]

    outgoing = front(prompt_input, next_input, norm_gain, w_key, w_value, w_query, key_offset, slots, sub)
    arrived = lax.all_to_all(
        outgoing, SP, split_axis=0, concat_axis=0, tiled=True, axis_index_groups=[order]
    )
    arrived = on_chip(arrived)
    own = join( arrived, heads, sub)
    tp_order = [(r + TP_FIRST) % heads for r in range(heads)]
    reading = lax.all_to_all(own, TP, split_axis=0, concat_axis=0, tiled=True, axis_index_groups=[tp_order])
    return finish(on_chip(reading), arrived, sub)


def solution(mesh):
    return jax.shard_map(
        shards,
        mesh=mesh,
        in_specs=(P(SP, None), P(), P(), P(None, TP), P(None, TP), P(None, TP), P(SP, TP)),
        out_specs=(P(SP, None, None, TP), P(SP, None, None, TP), P()),
        check_vma=False,
    )
```
